32 devices in a mesh: fs: 8 (over z, core), tp: 4 (over y, x).
Axes of the slice: x: 2, y: 2, z: 4, core: 2. Of those that a mesh axis runs over, the one named last changes fastest.
Arguments:
- tokens: bfloat16 [1024, 2048], P('fs'), may hold values from -6 to 6
- experts: int32 [1024, 4], P('fs'), may hold values from 0 to 7, all different within a row; in each aligned block of 128 rows (0 to 127, 128 to 255, ...) at most 96 rows name the same one
- routing: float32 [1024, 4], P('fs'), may hold values from 0.05 to 0.6
- norm_gain: float32 [2048], replicated, may hold values from 0.1 to 1.9
- gate_master: float32 [8, 2048, 2048], P(None, 'fs', 'tp'), may hold values from -0.625 to 0.625
- linear_master: float32 [8, 2048, 2048], P(None, 'fs', 'tp'), may hold values from -0.625 to 0.625
- down_weight: bfloat16 [8, 2048, 2048], P('fs', None, 'tp'), may hold values from -0.013671875 to 0.013671875
Outputs:
- gate_out: bfloat16 [8, 2048, 2048], P('fs', None, 'tp')
- linear_out: bfloat16 [8, 2048, 2048], P('fs', None, 'tp')
- expert_mix: bfloat16 [1024, 2048], P('fs', 'tp')
The draws below stay inside these ranges and needn't reach their ends.
Inputs may be any that keep to these rules, and one draw needn't show every extreme that they name: Each row names 4 different experts; within the rows of one index of fs (aligned blocks of 128 rows) no expert is named by more than 96 rows, and in some blocks some expert is named by exactly 96; every expert is named somewhere.
All inputs are finite; a program needn't handle non-finite values.
Results may differ from the reference program's by a relative error of at most 0.023.
Values may be sent and summed in bfloat16 or wider, within the bound.
A program may use at most 64 MiB of HBM per device.

```python
import math
import jax
import jax.numpy as jnp
import numpy as np
from jax import lax

D = 2048
DE = 2048
TOP = 4
TOK_DEV = 128
EXPERTS = 8
HID_DEV = 512
CAP = 96
TOKENS = 1024
N_TP = 4


def levels(key, dims, shards, smallest, largest):
    level = 1.0
    for position, blocks in shards:
        draws = jax.random.uniform(jax.random.fold_in(jax.random.fold_in(key, 6), position), (blocks,), jnp.float32, smallest / len(shards), largest / len(shards))
        level = level * jnp.repeat(jnp.exp(draws), dims[position] // blocks).reshape((-1,) + (1,) * (len(dims) - 1 - position))
    return level


def assign_block(own_key, own, number, rows, count, top, most, lean):
    sequence = jax.random.permutation(own_key, count)
    packed, usual = shares(count, rows * top, most, lean, True), shares(count, rows * top, most, lean, False)
    places = jnp.arange(count)

    def named(tallies, offset_by):
        used = int((tallies > 0).sum())
        fixed = max(1, used // 4)
        moved = fixed + (places - fixed + offset_by * (used - fixed)) % max(1, count - fixed)
        return jnp.zeros((count,), jnp.int32).at[sequence[jnp.where(places < fixed, places, moved)]].set(jnp.asarray(tallies, jnp.int32))

    tallies = jnp.where(number % 4 == 0, named(packed, number // 4), named(usual, number - number // 4 - 1))
    mixed = jax.random.permutation(jax.random.fold_in(own, 3), count)
    donor, sink = mixed[0:count // 2 * 2:2], mixed[1:count // 2 * 2:2]
    room = jnp.minimum(tallies[donor] - 1, most - tallies[sink]) // 2
    room = jnp.where((donor == sequence[0]) | (sink == sequence[0]) | (tallies[sink] == 0), 0, jnp.maximum(room, 0))
    moved = jax.random.randint(jax.random.fold_in(own, 4), (count // 2,), 0, 1 << 20) % (room + 1)
    tallies = tallies.at[donor].add(-moved).at[sink].add(moved)
    labels = jnp.searchsorted(jnp.cumsum(tallies), jnp.arange(rows * top), side="right").astype(jnp.int32)
    listing = labels.reshape(top, rows).T
    listing = listing[jax.random.permutation(jax.random.fold_in(own, 1), rows)]
    offset_by = jax.random.randint(jax.random.fold_in(own, 2), (rows, 1), 0, top)
    return jnp.take_along_axis(listing, (jnp.arange(top)[None, :] + offset_by) % top, axis=1)


def shares(number_of, total, limit, lean, full):
    loads = [(1 << 20) // math.isqrt(rank ** lean) + 1 for rank in range(1, number_of + 1)]
    largest = limit if full else min(limit, max(-(-total // number_of), total * loads[0] // sum(loads)))
    least = 1 if total - largest >= number_of - 1 else 0
    given, surplus = [largest] + [least] * (number_of - 1), total - largest - least * (number_of - 1)
    while surplus > 0:
        movable = [i for i in range(1, number_of) if given[i] < largest] or [i for i in range(1, number_of) if given[i] < limit]
        mass, budget = sum([loads[i] for i in movable]), surplus
        for i in movable:
            extra = min(limit - given[i], max(1, budget * loads[i] // mass), surplus)
            given[i] = given[i] + extra
            surplus = surplus - extra
    return np.array(given)


def centred(stream_key, shape, scale, bound, shards=(), kind=jnp.bfloat16):
    loudness = levels(stream_key, shape, shards, -0.22, 0.18) if shards else 1.0
    entries = jax.random.normal(stream_key, shape, jnp.float32) * scale * loudness
    return jnp.minimum(jnp.maximum(entries, -bound), bound).astype(kind)


def setup_inputs(seed: int = 0) -> dict:
    key_list = jax.random.split(jax.random.key(seed), 8)
    tokens = centred(key_list[0], (TOKENS, D), 1.0, 6.0, ((0, 8),))
    experts_keys = jax.random.split(jax.random.fold_in(key_list[1], 1), TOKENS // TOK_DEV)
    experts_turns = jax.random.permutation(jax.random.fold_in(key_list[1], 3), TOKENS // TOK_DEV)
    experts = jax.vmap(lambda own, number: assign_block(jax.random.fold_in(key_list[1], 2), own, number, TOK_DEV, EXPERTS, TOP, CAP, 0))(experts_keys, experts_turns).reshape((TOKENS, TOP))
    routing = jnp.clip(0.05 + 0.55 * jax.random.uniform(key_list[2], (TOKENS, TOP), jnp.float32) ** levels(key_list[2], (TOKENS, TOP), ((0, 8),), -0.2, 0.2), 0.05, 0.6)
    norm_gain = jnp.clip(1.0 + 0.18 * jax.random.normal(key_list[3], (D,), jnp.float32), 0.1, 1.9)
    gate_master = centred(key_list[4], (EXPERTS, D, DE), (D // 25) ** -0.5, 0.625, ((1, 8), (2, 4)), jnp.float32)
    linear_master = centred(key_list[5], (EXPERTS, D, DE), (D // 25) ** -0.5, 0.625, ((1, 8), (2, 4)), jnp.float32)
    down_weight = centred(key_list[6], (EXPERTS, D, DE), (DE * 100) ** -0.5, 0.013671875, ((0, 8), (2, 4)))
    return dict(tokens=tokens, experts=experts, routing=routing, norm_gain=norm_gain, gate_master=gate_master, linear_master=linear_master, down_weight=down_weight)


clamp_limit = 7.0
gate_slope = 1.702


def reference(tokens, experts, routing, norm_gain, gate_master, linear_master, down_weight):
    gain_col = norm_gain[None, :, None]
    gate_out = (gate_master * gain_col).astype(jnp.bfloat16)
    linear_out = (linear_master * gain_col).astype(jnp.bfloat16)
    flat_ids = experts.reshape(-1)
    owner = jnp.arange(TOKENS * TOP, dtype=jnp.int32) // TOP
    weights = routing.reshape(-1)
    span_rows = CAP * EXPERTS

    def one_expert(running, expert_id):
        pick_order = jnp.argsort((flat_ids != expert_id).astype(jnp.int32), stable=True)[:span_rows]
        in_use = flat_ids[pick_order] == expert_id
        row_owner = owner[pick_order]
        row_data = tokens[row_owner]
        pre_gate = jnp.dot(row_data, gate_out[expert_id], preferred_element_type=jnp.float32)
        pre_linear = jnp.dot(row_data, linear_out[expert_id], preferred_element_type=jnp.float32)
        clamped = jnp.minimum(pre_gate, clamp_limit)
        active = (clamped * jax.nn.sigmoid(gate_slope * clamped)
                  * (jnp.clip(pre_linear, -clamp_limit, clamp_limit) + 1.0)).astype(jnp.bfloat16)
        blocks = active.astype(jnp.float32).reshape(span_rows, N_TP, HID_DEV)
        down_blocks = down_weight[expert_id].astype(jnp.float32).reshape(D, N_TP, HID_DEV)
        block_part = jnp.einsum("rbh,dbh->rbd", blocks, down_blocks)
        rounded = lax.optimization_barrier(block_part.astype(jnp.bfloat16)).astype(jnp.float32)
        total = jnp.sum(rounded, axis=1)
        scale_rows = jnp.where(in_use, weights[pick_order], jnp.float32(0.0))
        running = running.at[row_owner].add(total * scale_rows[:, None])
        return running, None

    start = jnp.zeros((TOKENS, D), jnp.float32)
    final, _ = lax.scan(one_expert, start, jnp.arange(EXPERTS, dtype=jnp.int32))
    return (gate_out, linear_out, final.astype(jnp.bfloat16))
```

```python
import jax
import jax.numpy as jnp
from jax import lax
from jax.sharding import PartitionSpec as P

clamp_limit = 7.0
gate_slope = 1.702


def solution(mesh):
    n_fs, n_tp = mesh.shape["fs"], mesh.shape["tp"]

    def on_device(tokens, experts, routing, norm_gain, gate_master, linear_master, down_weight):
        expert_count, depth, _ = gate_master.shape
        width = tokens.shape[1]
        fs, tp = lax.axis_index("fs"), lax.axis_index("tp")
        cols = width // n_tp
        mine = lax.dynamic_slice_in_dim(tokens, tp * cols, cols, axis=1)
        quarter = lax.all_gather(mine, "fs", axis=0, tiled=True)
        everyone = lax.all_gather(quarter, "tp", axis=1, tiled=True)
        choice = experts[:, :, None] == jnp.arange(expert_count, dtype=jnp.int32)[None, None, :]
        share = jnp.sum(jnp.where(choice, routing[:, :, None], 0.0), axis=1)
        shares = lax.all_gather(share, "fs", axis=0, tiled=True)
        share_mine = lax.dynamic_slice_in_dim(shares, fs, 1, axis=1)
        gain = lax.dynamic_slice_in_dim(norm_gain, fs * depth, depth, axis=0)[None, :, None]
        gate_out, linear_out = (
            lax.all_to_all(
                (master * gain).astype(jnp.bfloat16), "fs", split_axis=0, concat_axis=1, tiled=True
            )
            for master in (gate_master, linear_master)
        )
        pre_gate = jnp.dot(everyone, gate_out[0], preferred_element_type=jnp.float32)
        pre_linear = jnp.dot(everyone, linear_out[0], preferred_element_type=jnp.float32)
        clamped = jnp.minimum(pre_gate, clamp_limit)
        active = (
            clamped
            * jax.nn.sigmoid(gate_slope * clamped)
            * (jnp.clip(pre_linear, -clamp_limit, clamp_limit) + 1.0)
        ).astype(jnp.bfloat16)
        part = lax.dot_general(
            active, down_weight[0], (((1,), (1,)), ((), ())), preferred_element_type=jnp.float32
        )
        part = (part * share_mine).astype(jnp.bfloat16)
        summed = lax.psum_scatter(part, "tp", scatter_dimension=1, tiled=True)
        mixed = lax.psum_scatter(summed, "fs", scatter_dimension=0, tiled=True)
        return (gate_out, linear_out, mixed)

    placed = (
        P("fs", None),
        P("fs", None),
        P("fs", None),
        P(),
        P(None, "fs", "tp"),
        P(None, "fs", "tp"),
        P("fs", None, "tp"),
    )
    return jax.shard_map(
        on_device,
        mesh=mesh,
        in_specs=placed,
        out_specs=(P("fs", None, "tp"), P("fs", None, "tp"), P("fs", "tp")),
        check_vma=False,
    )
```

```python
import functools

import jax
import jax.numpy as jnp
from jax import lax
from jax.experimental import pallas as pl
from jax.experimental.pallas import tpu as pltpu
from jax.sharding import PartitionSpec as P

clamp_limit = 7.0
gate_slope = 1.702
CORES = 2
LANES = 128
MESH = pl.DeviceIdType.MESH
F32, BF16 = jnp.float32, jnp.bfloat16


def loop(lo, hi, body):
    if hi - lo <= 8:
        for k in range(lo, hi):
            body(k)
    else:
        lax.fori_loop(lo, hi, lambda k, c: (body(k), c)[1], 0)


def kernel(
    n_fs, n_tp, n_chunks,
    tokens_ref, share_ref, gain_ref, gate_ref, linear_ref, down_ref,
    gate_out, linear_out, mix_out,
    toks, stage_g, stage_l, wsend, wrecv, dts, acts, acc, shares,
    osend, orecv, zsend, zrecv,
    local_sem, stage_sem, own_sem, out_sem, dl_sem,
    w_s, w_r, s_s, s_r, t1_s, t1_r, t2_s, t2_r, t3_s, t3_r,
    d_s, d_r, a_s, a_r, o_s, o_r, z_s, z_r,
):
    fs, tp = lax.axis_index("fs"), lax.axis_index("tp")
    n_z = n_fs // CORES
    z, core = fs // CORES, lax.rem(fs, CORES)
    partner = z * CORES + (1 - core)
    tok, width = tokens_ref.shape
    experts, depth, cols = gate_ref.shape
    qcols = width // n_tp
    dcols = width // n_tp
    ch = cols // n_chunks

    def ds(i, n):
        return pl.ds(pl.multiple_of(i * n, n), n)

    def remote(src, dst, ss, rs, where):
        return pltpu.make_async_remote_copy(
            src_ref=src, dst_ref=dst, send_sem=ss, recv_sem=rs,
            device_id=where, device_id_type=MESH,
        )

    def peer_fs(k):
        return {"fs": lax.rem(fs + k, n_fs), "tp": tp}

    def peer_z(k):
        return {"fs": lax.rem(z + k, n_z) * CORES + core, "tp": tp}

    def peer_tp(k):
        return {"fs": fs, "tp": lax.rem(tp + k, n_tp)}

    over = {"fs": partner, "tp": tp}

    def stage(j):
        slot = j % 2
        c = pl.ds(j * ch, ch)
        return (
            pltpu.make_async_copy(gate_ref.at[:, :, c], stage_g.at[slot], stage_sem.at[0, slot]),
            pltpu.make_async_copy(linear_ref.at[:, :, c], stage_l.at[slot], stage_sem.at[1, slot]),
        )

    def src_fs(kz):
        return lax.rem(z + n_z - kz, n_z) * CORES + core

    def w_copy(j, k):
        to = lax.rem(fs + k, n_fs)
        return remote(wsend.at[j, to], wrecv.at[j, ds(fs, depth)], w_s.at[j, k], w_r.at[j, k], peer_fs(k))

    def w_own(j):
        return pltpu.make_async_copy(wsend.at[j, fs], wrecv.at[j, ds(fs, depth)], own_sem.at[j])

    def s_copy(k):
        return remote(share_ref, shares.at[fs], s_s.at[k], s_r.at[k], peer_fs(k))

    def t1_copy(k):
        block = toks.at[ds(fs, tok), ds(tp, qcols)]
        return remote(block, block, t1_s.at[k], t1_r.at[k], peer_z(k))

    def t2_copy(kz, k):
        block = toks.at[ds(src_fs(kz), tok), ds(tp, qcols)]
        return remote(block, block, t2_s.at[kz, k], t2_r.at[kz, k], peer_tp(k))

    def t3_copy(kz):
        block = toks.at[ds(src_fs(kz), tok)]
        return remote(block, block, t3_s.at[kz], t3_r.at[kz], over)

    def d_copy(j, k):
        to = lax.rem(tp + k, n_tp)
        return remote(
            down_ref.at[0, ds(to, dcols), pl.ds(j * ch, ch)],
            dts.at[j, :, ds(tp, ch)], d_s.at[j, k], d_r.at[j, k], peer_tp(k),
        )

    def d_own(j):
        return pltpu.make_async_copy(
            down_ref.at[0, ds(tp, dcols), pl.ds(j * ch, ch)], dts.at[j, :, ds(tp, ch)], dl_sem.at[j]
        )

    def a_copy(j, k):
        block = acts.at[j, :, ds(tp, ch)]
        return remote(block, block, a_s.at[j, k], a_r.at[j, k], peer_tp(k))

    def outs(j):
        c = pl.ds(j * ch, ch)
        return (
            pltpu.make_async_copy(wrecv.at[j, :, pl.ds(0, ch)], gate_out.at[0, :, c], out_sem.at[0, j]),
            pltpu.make_async_copy(wrecv.at[j, :, pl.ds(ch, ch)], linear_out.at[0, :, c], out_sem.at[1, j]),
        )

    def o_copy(kz):
        return remote(osend.at[kz], orecv.at[kz], o_s.at[kz], o_r.at[kz], over)

    def z_copy(kz):
        return remote(zsend.at[kz], zrecv.at[kz], z_s.at[kz], z_r.at[kz], peer_z(kz))

    own_tokens = pltpu.make_async_copy(tokens_ref, toks.at[ds(fs, tok)], local_sem.at[0])
    own_share = pltpu.make_async_copy(share_ref, shares.at[fs], local_sem.at[1])
    for c in (own_tokens, own_share, *stage(0)):
        c.start()

    barrier = pltpu.get_barrier_semaphore()
    loop(1, n_fs, lambda k: pl.semaphore_signal(barrier, inc=1, device_id=peer_fs(k), device_id_type=MESH))
    loop(1, n_tp, lambda k: pl.semaphore_signal(barrier, inc=1, device_id=peer_tp(k), device_id_type=MESH))
    pl.semaphore_wait(barrier, n_fs + n_tp - 2)

    own_tokens.wait()
    loop(1, n_z, lambda k: t1_copy(k).start())
    loop(1, n_fs, lambda k: s_copy(k).start())
    early = (n_chunks + 1) // 2
    for j in range(early):
        d_own(j).start()
        loop(1, n_tp, lambda k: d_copy(j, k).start())

    half = n_fs // 2
    for j in range(n_chunks):
        for c in stage(j):
            c.wait()
        if j + 1 < n_chunks:
            for c in stage(j + 1):
                c.start()

        def cast(e, carry):
            wsend[j, e, :, 0:ch] = (stage_g[j % 2, e] * gain_ref[...]).astype(BF16)
            wsend[j, e, :, ch:] = (stage_l[j % 2, e] * gain_ref[...]).astype(BF16)
            return carry

        lax.fori_loop(0, experts, cast, 0)
        loop(0, half, lambda i: w_copy(j, half - i).start())
        loop(half + 1, n_fs, lambda k: w_copy(j, k).start())
        w_own(j).start()

    def spread(kz):
        if not (isinstance(kz, int) and kz == 0):
            t1_copy(kz).wait_recv()
        loop(1, n_tp, lambda k: t2_copy(kz, k).start())

    loop(1, n_z, spread)
    for j in range(early, n_chunks):
        d_own(j).start()
        loop(1, n_tp, lambda k: d_copy(j, k).start())
    t3_copy(0).start()

    def join(kz):
        loop(1, n_tp, lambda k: t2_copy(kz, k).wait_recv())
        t3_copy(kz).start()

    loop(1, n_z, join)
    loop(0, n_z, lambda kz: t3_copy(kz).wait_recv())

    total = n_fs * tok
    rows = min(total, 256)

    def down(j):
        d_own(j).wait()
        loop(1, n_tp, lambda k: d_copy(j, k).wait_recv())
        loop(1, n_tp, lambda k: a_copy(j, k).wait_recv())

    def product(j, r):
        return lax.dot_general(
            acts[j, r, :], dts[j], (((1,), (1,)), ((), ())), preferred_element_type=F32
        )

    def accumulate(j):
        down(j)

        def step(i, carry):
            r = ds(i, rows)
            if j == 0:
                acc[r, :] = product(j, r)
            else:
                acc[r, :] += product(j, r)
            return carry

        lax.fori_loop(0, total // rows, step, 0)

    for j in range(n_chunks):
        w_own(j).wait()
        loop(1, n_fs, lambda k: w_copy(j, k).wait_recv())
        for c in outs(j):
            c.start()

        def up(i, carry):
            r = ds(i, rows)
            pre = jnp.dot(toks[r, :], wrecv[j], preferred_element_type=F32)
            c = jnp.minimum(pre[:, 0:ch], clamp_limit)
            lin = jnp.clip(pre[:, ch:], -clamp_limit, clamp_limit) + 1.0
            acts[j, r, ds(tp, ch)] = (c * jax.nn.sigmoid(gate_slope * c) * lin).astype(BF16)
            return carry

        lax.fori_loop(0, total // rows, up, 0)
        loop(1, n_tp, lambda k: a_copy(j, k).start())
        if j > 0:
            accumulate(j - 1)

    own_share.wait()
    loop(1, n_fs, lambda k: s_copy(k).wait_recv())
    last = n_chunks - 1
    down(last)

    def weighted(who):
        r = ds(who, tok)
        value = product(last, r)
        if last > 0:
            value = value + acc[r, :]
        line = shares[who, pl.ds(fs, 1), :]
        w = jnp.transpose(jnp.broadcast_to(line, (tok, tok)))
        return value * jnp.concatenate([w] * (dcols // LANES), axis=1)

    def give(kz):
        to = lax.rem(z + kz, n_z) * CORES + (1 - core)
        osend[kz] = weighted(to).astype(BF16)
        o_copy(kz).start()

    def keep(kz):
        to = lax.rem(z + kz, n_z) * CORES + core
        acc[ds(to, tok), :] = weighted(to)

    def pass_on(kz):
        to = lax.rem(z + kz, n_z) * CORES + core
        o_copy(kz).wait_recv()
        zsend[kz] = (acc[ds(to, tok), :] + orecv[kz].astype(F32)).astype(BF16)
        z_copy(kz).start()

    loop(1, n_z, give)
    give(0)
    loop(1, n_z, keep)
    keep(0)
    loop(1, n_z, pass_on)
    o_copy(0).wait_recv()
    r = ds(fs, tok)
    acc[r, :] += orecv[0].astype(F32)

    def gather(kz):
        z_copy(kz).wait_recv()
        acc[r, :] += zrecv[kz].astype(F32)

    loop(1, n_z, gather)
    mix_out[...] = acc[r, :].astype(BF16)

    for j in range(n_chunks):
        for c in outs(j):
            c.wait()
        loop(1, n_fs, lambda k: w_copy(j, k).wait_send())
        loop(1, n_tp, lambda k: d_copy(j, k).wait_send())
        loop(1, n_tp, lambda k: a_copy(j, k).wait_send())
    loop(1, n_fs, lambda k: s_copy(k).wait_send())
    loop(1, n_z, lambda k: t1_copy(k).wait_send())
    loop(1, n_z, lambda kz: loop(1, n_tp, lambda k: t2_copy(kz, k).wait_send()))
    loop(0, n_z, lambda kz: t3_copy(kz).wait_send())
    loop(0, n_z, lambda kz: o_copy(kz).wait_send())
    loop(1, n_z, lambda kz: z_copy(kz).wait_send())


def solution(mesh):
    n_fs, n_tp = mesh.shape["fs"], mesh.shape["tp"]

    def on_device(tokens, experts, routing, norm_gain, gate_master, linear_master, down_weight):
        expert_count, depth, cols = gate_master.shape
        tok, width = tokens.shape
        n_z = n_fs // CORES
        ch = min(LANES, cols)
        n_chunks = cols // ch
        dcols = width // n_tp
        fs = lax.axis_index("fs")
        choice = experts.T[:, None, :] == jnp.arange(expert_count, dtype=jnp.int32)[None, :, None]
        share = jnp.sum(jnp.where(choice, routing.T[:, None, :], 0.0), axis=0)
        gain = lax.dynamic_slice_in_dim(norm_gain, fs * depth, depth, axis=0)
        gain = jnp.broadcast_to(gain[:, None], (depth, ch))
        hbm = pl.BlockSpec(memory_space=pl.ANY)
        vmem = pl.BlockSpec(memory_space=pltpu.VMEM)
        dma = pltpu.SemaphoreType.DMA
        slots = min(2, n_chunks)
        out_shape = jax.ShapeDtypeStruct((1, width, cols), BF16)
        pairs = [
            (n_chunks, n_fs), (n_fs,), (n_z,), (n_z, n_tp), (n_z,),
            (n_chunks, n_tp), (n_chunks, n_tp), (n_z,), (n_z,),
        ]
        return pl.pallas_call(
            functools.partial(kernel, n_fs, n_tp, n_chunks),
            out_shape=(out_shape, out_shape, jax.ShapeDtypeStruct((tok, dcols), BF16)),
            in_specs=[hbm, vmem, vmem, hbm, hbm, hbm],
            out_specs=(hbm, hbm, vmem),
            scratch_shapes=[
                pltpu.VMEM((n_fs * tok, width), BF16),
                pltpu.VMEM((slots, expert_count, depth, ch), F32),
                pltpu.VMEM((slots, expert_count, depth, ch), F32),
                pltpu.VMEM((n_chunks, expert_count, depth, 2 * ch), BF16),
                pltpu.VMEM((n_chunks, width, 2 * ch), BF16),
                pltpu.VMEM((n_chunks, dcols, n_tp * ch), BF16),
                pltpu.VMEM((n_chunks, n_fs * tok, n_tp * ch), BF16),
                pltpu.VMEM((n_fs * tok, dcols), F32),
                pltpu.VMEM((n_fs, expert_count, tok), F32),
                pltpu.VMEM((n_z, tok, dcols), BF16),
                pltpu.VMEM((n_z, tok, dcols), BF16),
                pltpu.VMEM((n_z, tok, dcols), BF16),
                pltpu.VMEM((n_z, tok, dcols), BF16),
                dma((2,)), dma((2, slots)), dma((n_chunks,)), dma((2, n_chunks)), dma((n_chunks,)),
            ] + [dma(shape) for shape in pairs for _ in range(2)],
            compiler_params=pltpu.CompilerParams(collective_id=0, has_side_effects=True),
        )(tokens, share, gain, gate_master, linear_master, down_weight)

    placed = (
        P("fs", None),
        P("fs", None),
        P("fs", None),
        P(),
        P(None, "fs", "tp"),
        P(None, "fs", "tp"),
        P("fs", None, "tp"),
    )
    return jax.shard_map(
        on_device,
        mesh=mesh,
        in_specs=placed,
        out_specs=(P("fs", None, "tp"), P("fs", None, "tp"), P("fs", "tp")),
        check_vma=False,
    )
```

```python
import functools

import jax
import jax.numpy as jnp
from jax import lax
from jax.experimental import pallas as pl
from jax.experimental.pallas import tpu as pltpu
from jax.sharding import PartitionSpec as P

clamp_limit = 7.0
gate_slope = 1.702
CORES = 2
LANES = 128
MESH = pl.DeviceIdType.MESH
F32, BF16 = jnp.float32, jnp.bfloat16


def loop(lo, hi, body):
    if hi - lo <= 8:
        for k in range(lo, hi):
            body(k)
    else:
        lax.fori_loop(lo, hi, lambda k, c: (body(k), c)[1], 0)


def kernel(
    n_fs, n_tp, n_chunks,
    tokens_ref, experts_ref, routing_ref, gain_ref, gate_ref, linear_ref, down_ref,
    gate_out, linear_out, mix_out,
    toks, gains, stage_g, stage_l, wsend, wrecv, dts, acts, acc, shares,
    osend, orecv, zsend, zrecv,
    local_sem, stage_sem, own_sem, out_sem, dl_sem,
    w_s, w_r, s_s, s_r, t1_s, t1_r, t2_s, t2_r, t3_s, t3_r,
    d_s, d_r, a_s, a_r, l_s, l_r, o_s, o_r, z_s, z_r,
):
    fs, tp = lax.axis_index("fs"), lax.axis_index("tp")
    n_z = n_fs // CORES
    z, core = fs // CORES, lax.rem(fs, CORES)
    partner = z * CORES + (1 - core)
    tok, width = tokens_ref.shape
    experts, depth, cols = gate_ref.shape
    qcols = width // n_tp
    dcols = width // n_tp
    ch = cols // n_chunks

    def ds(i, n):
        return pl.ds(pl.multiple_of(i * n, n), n)

    def remote(src, dst, ss, rs, where):
        return pltpu.make_async_remote_copy(
            src_ref=src, dst_ref=dst, send_sem=ss, recv_sem=rs,
            device_id=where, device_id_type=MESH,
        )

    def peer_fs(k):
        return {"fs": lax.rem(fs + k, n_fs), "tp": tp}

    def peer_z(k):
        return {"fs": lax.rem(z + k, n_z) * CORES + core, "tp": tp}

    def peer_tp(k):
        return {"fs": fs, "tp": lax.rem(tp + k, n_tp)}

    over = {"fs": partner, "tp": tp}

    def stage(j):
        slot = j % 2
        c = pl.ds(j * ch, ch)
        return (
            pltpu.make_async_copy(gate_ref.at[:, :, c], stage_g.at[slot], stage_sem.at[0, slot]),
            pltpu.make_async_copy(linear_ref.at[:, :, c], stage_l.at[slot], stage_sem.at[1, slot]),
        )

    def src_fs(kz):
        return lax.rem(z + n_z - kz, n_z) * CORES + core

    def w_copy(j, k):
        to = lax.rem(fs + k, n_fs)
        return remote(wsend.at[j, to], wrecv.at[j, ds(fs, depth)], w_s.at[j, k], w_r.at[j, k], peer_fs(k))

    def w_own(j):
        return pltpu.make_async_copy(wsend.at[j, fs], wrecv.at[j, ds(fs, depth)], own_sem.at[j])

    def s_copy(k):
        return remote(shares.at[fs], shares.at[fs], s_s.at[k], s_r.at[k], peer_fs(k))

    def t1_copy(k):
        block = toks.at[ds(fs, tok), ds(tp, qcols)]
        return remote(block, block, t1_s.at[k], t1_r.at[k], peer_z(k))

    def t2_copy(kz, k):
        block = toks.at[ds(src_fs(kz), tok), ds(tp, qcols)]
        return remote(block, block, t2_s.at[kz, k], t2_r.at[kz, k], peer_tp(k))

    def t3_copy(kz):
        block = toks.at[ds(src_fs(kz), tok)]
        return remote(block, block, t3_s.at[kz], t3_r.at[kz], over)

    def d_copy(j, k):
        to = lax.rem(tp + k, n_tp)
        return remote(
            down_ref.at[0, ds(to, dcols), pl.ds(j * ch, ch)],
            dts.at[j, :, ds(tp, ch)], d_s.at[j, k], d_r.at[j, k], peer_tp(k),
        )

    def d_own(j):
        return pltpu.make_async_copy(
            down_ref.at[0, ds(tp, dcols), pl.ds(j * ch, ch)], dts.at[j, :, ds(tp, ch)], dl_sem.at[j]
        )

    def a_copy(j, k):
        block = acts.at[j, :, ds(tp, ch)]
        return remote(block, block, a_s.at[j, k], a_r.at[j, k], peer_tp(k))

    def outs(j):
        c = pl.ds(j * ch, ch)
        return (
            pltpu.make_async_copy(wrecv.at[j, :, pl.ds(0, ch)], gate_out.at[0, :, c], out_sem.at[0, j]),
            pltpu.make_async_copy(wrecv.at[j, :, pl.ds(ch, ch)], linear_out.at[0, :, c], out_sem.at[1, j]),
        )

    def o_copy(kz):
        return remote(osend.at[kz], orecv.at[kz], o_s.at[kz], o_r.at[kz], over)

    def zx(m):
        out, bit = z, 1
        while bit <= m:
            if m & bit:
                out = out + bit - 2 * bit * lax.rem(z // bit, 2)
            bit *= 2
        return out

    def l_copy(m, k):
        block = acts.at[n_chunks - 1, ds(zx(m), CORES * tok), ds(tp, ch)]
        return remote(block, block, l_s.at[m, k], l_r.at[m, k], peer_tp(k))

    def z_copy(m):
        where = {"fs": zx(m) * CORES + core, "tp": tp}
        return remote(zsend.at[m], zrecv.at[m], z_s.at[m], z_r.at[m], where)

    own_tokens = pltpu.make_async_copy(tokens_ref, toks.at[ds(fs, tok)], local_sem.at[0])
    for c in (own_tokens, *stage(0)):
        c.start()

    barrier = pltpu.get_barrier_semaphore()
    loop(1, n_fs, lambda k: pl.semaphore_signal(barrier, inc=1, device_id=peer_fs(k), device_id_type=MESH))
    loop(1, n_tp, lambda k: pl.semaphore_signal(barrier, inc=1, device_id=peer_tp(k), device_id_type=MESH))

    lane = lax.broadcasted_iota(jnp.int32, (tok, LANES), 1)
    share = jnp.zeros((tok, LANES), F32)
    for k in range(experts_ref.shape[1]):
        share += jnp.where(experts_ref[:, k : k + 1] == lane, routing_ref[:, k : k + 1], 0.0)
    shares[fs] = jnp.transpose(share)[:experts]
    for i in range(max(depth // LANES, 1)):
        line = gain_ref[pl.ds(fs * depth // LANES + i, 1), :]
        gains[i * LANES : (i + 1) * LANES, :] = jnp.transpose(jnp.broadcast_to(line, (LANES, LANES)))
    gain_rows = pl.ds(pl.multiple_of(lax.rem(fs * depth, LANES), 8), depth)
    pl.semaphore_wait(barrier, n_fs + n_tp - 2)

    own_tokens.wait()
    loop(1, n_z, lambda k: t1_copy(k).start())
    early = (n_chunks + 1) // 2
    for j in range(early):
        d_own(j).start()
        loop(1, n_tp, lambda k: d_copy(j, k).start())

    loop(1, n_fs, lambda k: s_copy(k).start())
    half = n_fs // 2
    for j in range(n_chunks):
        for c in stage(j):
            c.wait()
        if j + 1 < n_chunks:
            for c in stage(j + 1):
                c.start()

        def cast(e, carry):
            wsend[j, e, :, 0:ch] = (stage_g[j % 2, e] * gains[gain_rows, 0:ch]).astype(BF16)
            wsend[j, e, :, ch:] = (stage_l[j % 2, e] * gains[gain_rows, 0:ch]).astype(BF16)
            return carry

        lax.fori_loop(0, experts, cast, 0)
        loop(0, half, lambda i: w_copy(j, half - i).start())
        loop(half + 1, n_fs, lambda k: w_copy(j, k).start())
        w_own(j).start()

    def spread(kz):
        if not (isinstance(kz, int) and kz == 0):
            t1_copy(kz).wait_recv()
        loop(1, n_tp, lambda k: t2_copy(kz, k).start())

    loop(1, n_z, spread)
    for j in range(early, n_chunks):
        d_own(j).start()
        loop(1, n_tp, lambda k: d_copy(j, k).start())
    t3_copy(0).start()

    def join(kz):
        loop(1, n_tp, lambda k: t2_copy(kz, k).wait_recv())
        t3_copy(kz).start()

    loop(1, n_z, join)
    loop(0, n_z, lambda kz: t3_copy(kz).wait_recv())

    total = n_fs * tok
    rows = min(total, 256)

    def down(j):
        d_own(j).wait()
        loop(1, n_tp, lambda k: d_copy(j, k).wait_recv())
        if j < n_chunks - 1:
            loop(1, n_tp, lambda k: a_copy(j, k).wait_recv())

    def product(j, r):
        return lax.dot_general(
            acts[j, r, :], dts[j], (((1,), (1,)), ((), ())), preferred_element_type=F32
        )

    def accumulate(j):
        down(j)

        def step(i, carry):
            r = ds(i, rows)
            if j == 0:
                acc[r, :] = product(j, r)
            else:
                acc[r, :] += product(j, r)
            return carry

        lax.fori_loop(0, total // rows, step, 0)

    def arrive(j):
        w_own(j).wait()
        loop(1, n_fs, lambda k: w_copy(j, k).wait_recv())
        for c in outs(j):
            c.start()

    def up(j, r):
        pre = jnp.dot(toks[r, :], wrecv[j], preferred_element_type=F32)
        c = jnp.minimum(pre[:, 0:ch], clamp_limit)
        lin = jnp.clip(pre[:, ch:], -clamp_limit, clamp_limit) + 1.0
        acts[j, r, ds(tp, ch)] = (c * jax.nn.sigmoid(gate_slope * c) * lin).astype(BF16)

    last = n_chunks - 1
    for j in range(last):
        arrive(j)
        lax.fori_loop(0, total // rows, lambda i, c: (up(j, ds(i, rows)), c)[1], 0)
        loop(1, n_tp, lambda k: a_copy(j, k).start())
        if j > 0:
            accumulate(j - 1)
    if last > 0:
        accumulate(last - 1)

    loop(1, n_fs, lambda k: s_copy(k).wait_recv())
    down(last)

    def weighted(who):
        r = ds(who, tok)
        value = product(last, r)
        if last > 0:
            value = value + acc[r, :]
        line = shares[who, pl.ds(fs, 1), :]
        w = jnp.transpose(jnp.broadcast_to(line, (tok, tok)))
        return value * jnp.concatenate([w] * (dcols // LANES), axis=1)

    def pass_on(m):
        r = ds(zx(m) * CORES + core, tok)
        o_copy(m).wait_recv()
        if m == 0:
            acc[r, :] += orecv[m].astype(F32)
        else:
            zsend[m] = (acc[r, :] + orecv[m].astype(F32)).astype(BF16)
            z_copy(m).start()

    order = list(range(n_z - 1, -1, -1))
    arrive(last)
    for m in order:
        up(last, ds(zx(m), CORES * tok))
        loop(1, n_tp, lambda k: l_copy(m, k).start())
    for m in order:
        loop(1, n_tp, lambda k: l_copy(m, k).wait_recv())
        osend[m] = weighted(zx(m) * CORES + (1 - core)).astype(BF16)
        o_copy(m).start()
        kept = zx(m) * CORES + core
        acc[ds(kept, tok), :] = weighted(kept)
        if m < n_z - 1:
            pass_on(m + 1)
    pass_on(0)
    r = ds(fs, tok)
    for m in order[:-1]:
        z_copy(m).wait_recv()
        acc[r, :] += zrecv[m].astype(F32)
    mix_out[...] = acc[r, :].astype(BF16)

    for j in range(n_chunks):
        for c in outs(j):
            c.wait()
        loop(1, n_fs, lambda k: w_copy(j, k).wait_send())
        loop(1, n_tp, lambda k: d_copy(j, k).wait_send())
        if j < last:
            loop(1, n_tp, lambda k: a_copy(j, k).wait_send())
    for m in order:
        loop(1, n_tp, lambda k: l_copy(m, k).wait_send())
    loop(1, n_fs, lambda k: s_copy(k).wait_send())
    loop(1, n_z, lambda k: t1_copy(k).wait_send())
    loop(1, n_z, lambda kz: loop(1, n_tp, lambda k: t2_copy(kz, k).wait_send()))
    loop(0, n_z, lambda kz: t3_copy(kz).wait_send())
    loop(0, n_z, lambda kz: o_copy(kz).wait_send())
    for m in order[:-1]:
        z_copy(m).wait_send()


def solution(mesh):
    n_fs, n_tp = mesh.shape["fs"], mesh.shape["tp"]

    def on_device(tokens, experts, routing, norm_gain, gate_master, linear_master, down_weight):
        expert_count, depth, cols = gate_master.shape
        tok, width = tokens.shape
        n_z = n_fs // CORES
        ch = min(LANES, cols)
        n_chunks = cols // ch
        dcols = width // n_tp
        lines = norm_gain.reshape(width // LANES, LANES)
        hbm = pl.BlockSpec(memory_space=pl.ANY)
        vmem = pl.BlockSpec(memory_space=pltpu.VMEM)
        dma = pltpu.SemaphoreType.DMA
        slots = min(2, n_chunks)
        out_shape = jax.ShapeDtypeStruct((1, width, cols), BF16)
        pairs = [
            (n_chunks, n_fs), (n_fs,), (n_z,), (n_z, n_tp), (n_z,),
            (n_chunks, n_tp), (n_chunks, n_tp), (n_z, n_tp), (n_z,), (n_z,),
        ]
        return pl.pallas_call(
            functools.partial(kernel, n_fs, n_tp, n_chunks),
            out_shape=(out_shape, out_shape, jax.ShapeDtypeStruct((tok, dcols), BF16)),
            in_specs=[hbm, vmem, vmem, vmem, hbm, hbm, hbm],
            out_specs=(hbm, hbm, vmem),
            scratch_shapes=[
                pltpu.VMEM((n_fs * tok, width), BF16),
                pltpu.VMEM((max(depth, LANES), LANES), F32),
                pltpu.VMEM((slots, expert_count, depth, ch), F32),
                pltpu.VMEM((slots, expert_count, depth, ch), F32),
                pltpu.VMEM((n_chunks, expert_count, depth, 2 * ch), BF16),
                pltpu.VMEM((n_chunks, width, 2 * ch), BF16),
                pltpu.VMEM((n_chunks, dcols, n_tp * ch), BF16),
                pltpu.VMEM((n_chunks, n_fs * tok, n_tp * ch), BF16),
                pltpu.VMEM((n_fs * tok, dcols), F32),
                pltpu.VMEM((n_fs, expert_count, tok), F32),
                pltpu.VMEM((n_z, tok, dcols), BF16),
                pltpu.VMEM((n_z, tok, dcols), BF16),
                pltpu.VMEM((n_z, tok, dcols), BF16),
                pltpu.VMEM((n_z, tok, dcols), BF16),
                dma((2,)), dma((2, slots)), dma((n_chunks,)), dma((2, n_chunks)), dma((n_chunks,)),
            ] + [dma(shape) for shape in pairs for _ in range(2)],
            compiler_params=pltpu.CompilerParams(collective_id=0, has_side_effects=True),
        )(tokens, experts, routing, lines, gate_master, linear_master, down_weight)

    placed = (
        P("fs", None),
        P("fs", None),
        P("fs", None),
        P(),
        P(None, "fs", "tp"),
        P(None, "fs", "tp"),
        P("fs", None, "tp"),
    )
    return jax.shard_map(
        on_device,
        mesh=mesh,
        in_specs=placed,
        out_specs=(P("fs", None, "tp"), P("fs", None, "tp"), P("fs", "tp")),
        check_vma=False,
    )
```

```python
import functools

import jax
import jax.numpy as jnp
from jax import lax
from jax.experimental import pallas as pl
from jax.experimental.pallas import tpu as pltpu
from jax.sharding import PartitionSpec as P

clamp_limit = 7.0
gate_slope = 1.702
CORES = 2
LANES = 128
MESH = pl.DeviceIdType.MESH
F32, BF16 = jnp.float32, jnp.bfloat16


def loop(lo, hi, body):
    if hi - lo <= 8:
        for k in range(lo, hi):
            body(k)
    else:
        lax.fori_loop(lo, hi, lambda k, c: (body(k), c)[1], 0)


def kernel(
    n_fs, n_tp, n_chunks,
    tokens_ref, experts_ref, routing_ref, gain_ref, gate_ref, linear_ref, down_ref,
    gate_out, linear_out, mix_out,
    toks, gains, stage_g, stage_l, wsend, wrecv, dts, acts, acc, shares,
    osend, orecv, zsend, zrecv,
    local_sem, stage_sem, own_sem, out_sem, dl_sem,
    w_s, w_r, s_s, s_r, t1_s, t1_r, t2_s, t2_r, t3_s, t3_r,
    d_s, d_r, a_s, a_r, l_s, l_r, o_s, o_r, z_s, z_r,
):
    fs, tp = lax.axis_index("fs"), lax.axis_index("tp")
    n_z = n_fs // CORES
    z, core = fs // CORES, lax.rem(fs, CORES)
    partner = z * CORES + (1 - core)
    across = n_z // 2
    tok, width = tokens_ref.shape
    experts, depth, cols = gate_ref.shape
    qcols = width // n_tp
    dcols = width // n_tp
    ch = cols // n_chunks

    def flip(index, mask):
        out, bit = index, 1
        while bit <= mask:
            if mask & bit:
                out = out + bit - 2 * bit * lax.rem(index // bit, 2)
            bit *= 2
        return out

    def zx(m):
        return flip(z, m)

    def ds(i, n):
        return pl.ds(pl.multiple_of(i * n, n), n)

    def remote(src, dst, ss, rs, where):
        return pltpu.make_async_remote_copy(
            src_ref=src, dst_ref=dst, send_sem=ss, recv_sem=rs,
            device_id=where, device_id_type=MESH,
        )

    def peer_fs(k):
        return {"fs": lax.rem(fs + k, n_fs), "tp": tp}

    def peer_tp(k):
        return {"fs": fs, "tp": lax.rem(tp + k, n_tp)}

    over = {"fs": partner, "tp": tp}

    def stage(j):
        slot = j % 2
        c = pl.ds(j * ch, ch)
        return (
            pltpu.make_async_copy(gate_ref.at[:, :, c], stage_g.at[slot], stage_sem.at[0, slot]),
            pltpu.make_async_copy(linear_ref.at[:, :, c], stage_l.at[slot], stage_sem.at[1, slot]),
        )

    def src_fs(m):
        return zx(m) * CORES + core

    def w_copy(j, k):
        to = flip(fs, k)
        return remote(
            wsend.at[j, to], wrecv.at[j, ds(fs, depth)], w_s.at[j, k], w_r.at[j, k], {"fs": to, "tp": tp}
        )

    def w_own(j):
        return pltpu.make_async_copy(wsend.at[j, fs], wrecv.at[j, ds(fs, depth)], own_sem.at[j])

    def s_copy(k):
        return remote(shares.at[fs], shares.at[fs], s_s.at[k], s_r.at[k], peer_fs(k))

    def t1_copy(m):
        block = toks.at[ds(fs if m <= across else src_fs(across), tok), ds(tp, qcols)]
        to = m if m <= across else m - across
        return remote(block, block, t1_s.at[m], t1_r.at[m], {"fs": src_fs(to), "tp": tp})

    def t2_copy(kz, k):
        block = toks.at[ds(src_fs(kz), tok), ds(tp, qcols)]
        return remote(block, block, t2_s.at[kz, k], t2_r.at[kz, k], peer_tp(k))

    def t3_copy(kz):
        block = toks.at[ds(src_fs(kz), tok)]
        return remote(block, block, t3_s.at[kz], t3_r.at[kz], over)

    def d_copy(j, k):
        to = lax.rem(tp + k, n_tp)
        return remote(
            down_ref.at[0, ds(to, dcols), pl.ds(j * ch, ch)],
            dts.at[j, :, ds(tp, ch)], d_s.at[j, k], d_r.at[j, k], peer_tp(k),
        )

    def d_own(j):
        return pltpu.make_async_copy(
            down_ref.at[0, ds(tp, dcols), pl.ds(j * ch, ch)], dts.at[j, :, ds(tp, ch)], dl_sem.at[j]
        )

    def a_copy(j, k):
        block = acts.at[j, :, ds(tp, ch)]
        return remote(block, block, a_s.at[j, k], a_r.at[j, k], peer_tp(k))

    def outs(j):
        c = pl.ds(j * ch, ch)
        return (
            pltpu.make_async_copy(wrecv.at[j, :, pl.ds(0, ch)], gate_out.at[0, :, c], out_sem.at[0, j]),
            pltpu.make_async_copy(wrecv.at[j, :, pl.ds(ch, ch)], linear_out.at[0, :, c], out_sem.at[1, j]),
        )

    def o_copy(kz):
        return remote(osend.at[kz], orecv.at[kz], o_s.at[kz], o_r.at[kz], over)

    def l_copy(m, k):
        block = acts.at[n_chunks - 1, ds(zx(m), CORES * tok), ds(tp, ch)]
        return remote(block, block, l_s.at[m, k], l_r.at[m, k], peer_tp(k))

    def z_copy(m):
        where = {"fs": zx(m) * CORES + core, "tp": tp}
        return remote(zsend.at[m], zrecv.at[m], z_s.at[m], z_r.at[m], where)

    own_tokens = pltpu.make_async_copy(tokens_ref, toks.at[ds(fs, tok)], local_sem.at[0])
    for c in (own_tokens, *stage(0)):
        c.start()

    barrier = pltpu.get_barrier_semaphore()
    loop(1, n_fs, lambda k: pl.semaphore_signal(barrier, inc=1, device_id=peer_fs(k), device_id_type=MESH))
    loop(1, n_tp, lambda k: pl.semaphore_signal(barrier, inc=1, device_id=peer_tp(k), device_id_type=MESH))

    expert = lax.broadcasted_iota(jnp.int32, (experts, tok), 0)
    share = jnp.zeros((experts, tok), F32)
    for k in range(experts_ref.shape[0]):
        share += jnp.where(experts_ref[k : k + 1, :] == expert, routing_ref[k : k + 1, :], 0.0)
    shares[fs] = share
    for i in range(max(depth // LANES, 1)):
        line = gain_ref[pl.ds(fs * depth // LANES + i, 1), :]
        gains[i * LANES : (i + 1) * LANES, :] = jnp.transpose(jnp.broadcast_to(line, (LANES, LANES)))
    gain_rows = pl.ds(pl.multiple_of(lax.rem(fs * depth, LANES), 8), depth)
    pl.semaphore_wait(barrier, n_fs + n_tp - 2)

    own_tokens.wait()
    for m in range(across, 0, -1):
        t1_copy(m).start()
    early = (n_chunks + 1) // 2
    for j in range(early):
        d_own(j).start()
        loop(1, n_tp, lambda k: d_copy(j, k).start())

    loop(1, n_fs, lambda k: s_copy(k).start())
    half = n_fs // 2

    def prepare(j):
        for c in stage(j):
            c.wait()
        if j + 1 < n_chunks:
            for c in stage(j + 1):
                c.start()

        def cast(e, carry):
            wsend[j, e, :, 0:ch] = (stage_g[j % 2, e] * gains[gain_rows, 0:ch]).astype(BF16)
            wsend[j, e, :, ch:] = (stage_l[j % 2, e] * gains[gain_rows, 0:ch]).astype(BF16)
            return carry

        lax.fori_loop(0, experts, cast, 0)
        w_own(j).start()
        for k in range(half - 1, 0, -1):
            w_copy(j, k).start()

    def spread(m):
        t1_copy(m).wait_recv()
        loop(1, n_tp, lambda k: t2_copy(m, k).start())

    crossing = list(range(n_fs - 1, half - 1, -1))
    prepare(0)
    for k in crossing[: half // 2]:
        w_copy(0, k).start()
    spread(across)
    for m in range(across + 1, n_z):
        t1_copy(m).start()
    for k in crossing[half // 2 :]:
        w_copy(0, k).start()
    t3_copy(0).start()
    for m in range(1, across):
        spread(m)
    for j in range(1, n_chunks):
        prepare(j)
    for j in range(1, n_chunks):
        for k in crossing:
            w_copy(j, k).start()
    for m in range(across + 1, n_z):
        spread(m)
    for j in range(early, n_chunks):
        d_own(j).start()
        loop(1, n_tp, lambda k: d_copy(j, k).start())
    for m in range(1, n_z):
        loop(1, n_tp, lambda k: t2_copy(m, k).wait_recv())
        t3_copy(m).start()
    for m in range(n_z):
        t3_copy(m).wait_recv()

    total = n_fs * tok
    rows = min(total, 256)

    def down(j):
        d_own(j).wait()
        loop(1, n_tp, lambda k: d_copy(j, k).wait_recv())
        if j < n_chunks - 1:
            loop(1, n_tp, lambda k: a_copy(j, k).wait_recv())

    def product(j, r):
        return lax.dot_general(
            acts[j, r, :], dts[j], (((1,), (1,)), ((), ())), preferred_element_type=F32
        )

    def accumulate(j):
        down(j)

        def step(i, carry):
            r = ds(i, rows)
            if j == 0:
                acc[r, :] = product(j, r)
            else:
                acc[r, :] += product(j, r)
            return carry

        lax.fori_loop(0, total // rows, step, 0)

    def arrive(j):
        w_own(j).wait()
        for k in range(1, n_fs):
            w_copy(j, k).wait_recv()
        for c in outs(j):
            c.start()

    def up(j, r):
        pre = jnp.dot(toks[r, :], wrecv[j], preferred_element_type=F32)
        c = jnp.minimum(pre[:, 0:ch], clamp_limit)
        lin = jnp.clip(pre[:, ch:], -clamp_limit, clamp_limit) + 1.0
        acts[j, r, ds(tp, ch)] = (c * jax.nn.sigmoid(gate_slope * c) * lin).astype(BF16)

    last = n_chunks - 1
    for j in range(last):
        arrive(j)
        lax.fori_loop(0, total // rows, lambda i, c: (up(j, ds(i, rows)), c)[1], 0)
        loop(1, n_tp, lambda k: a_copy(j, k).start())
        if j > 0:
            accumulate(j - 1)
    if last > 0:
        accumulate(last - 1)

    loop(1, n_fs, lambda k: s_copy(k).wait_recv())
    down(last)

    def weighted(who):
        r = ds(who, tok)
        value = product(last, r)
        if last > 0:
            value = value + acc[r, :]
        line = shares[who, pl.ds(fs, 1), :]
        w = jnp.transpose(jnp.broadcast_to(line, (tok, tok)))
        return value * jnp.concatenate([w] * (dcols // LANES), axis=1)

    def pass_on(m):
        r = ds(zx(m) * CORES + core, tok)
        o_copy(m).wait_recv()
        if m == 0:
            acc[r, :] += orecv[m].astype(F32)
        else:
            zsend[m] = (acc[r, :] + orecv[m].astype(F32)).astype(BF16)
            z_copy(m).start()

    order = list(range(n_z - 1, -1, -1))
    arrive(last)
    for m in order:
        up(last, ds(zx(m), CORES * tok))
        loop(1, n_tp, lambda k: l_copy(m, k).start())
    for m in order:
        loop(1, n_tp, lambda k: l_copy(m, k).wait_recv())
        osend[m] = weighted(zx(m) * CORES + (1 - core)).astype(BF16)
        o_copy(m).start()
        kept = zx(m) * CORES + core
        acc[ds(kept, tok), :] = weighted(kept)
        if m < n_z - 1:
            pass_on(m + 1)
    pass_on(0)
    r = ds(fs, tok)
    for m in order[:-1]:
        z_copy(m).wait_recv()
        acc[r, :] += zrecv[m].astype(F32)
    mix_out[...] = acc[r, :].astype(BF16)

    for j in range(n_chunks):
        for c in outs(j):
            c.wait()
        for k in range(1, n_fs):
            w_copy(j, k).wait_send()
        loop(1, n_tp, lambda k: d_copy(j, k).wait_send())
        if j < last:
            loop(1, n_tp, lambda k: a_copy(j, k).wait_send())
    for m in order:
        loop(1, n_tp, lambda k: l_copy(m, k).wait_send())
    loop(1, n_fs, lambda k: s_copy(k).wait_send())
    for m in range(n_z):
        if m > 0:
            t1_copy(m).wait_send()
            loop(1, n_tp, lambda k: t2_copy(m, k).wait_send())
        t3_copy(m).wait_send()
    loop(0, n_z, lambda kz: o_copy(kz).wait_send())
    for m in order[:-1]:
        z_copy(m).wait_send()


def solution(mesh):
    n_fs, n_tp = mesh.shape["fs"], mesh.shape["tp"]

    def on_device(tokens, experts, routing, norm_gain, gate_master, linear_master, down_weight):
        expert_count, depth, cols = gate_master.shape
        tok, width = tokens.shape
        n_z = n_fs // CORES
        ch = min(LANES, cols)
        n_chunks = cols // ch
        dcols = width // n_tp
        lines = norm_gain.reshape(width // LANES, LANES)
        hbm = pl.BlockSpec(memory_space=pl.ANY)
        vmem = pl.BlockSpec(memory_space=pltpu.VMEM)
        dma = pltpu.SemaphoreType.DMA
        slots = min(2, n_chunks)
        out_shape = jax.ShapeDtypeStruct((1, width, cols), BF16)
        pairs = [
            (n_chunks, n_fs), (n_fs,), (n_z,), (n_z, n_tp), (n_z,),
            (n_chunks, n_tp), (n_chunks, n_tp), (n_z, n_tp), (n_z,), (n_z,),
        ]
        return pl.pallas_call(
            functools.partial(kernel, n_fs, n_tp, n_chunks),
            out_shape=(out_shape, out_shape, jax.ShapeDtypeStruct((tok, dcols), BF16)),
            in_specs=[hbm, vmem, vmem, vmem, hbm, hbm, hbm],
            out_specs=(hbm, hbm, vmem),
            scratch_shapes=[
                pltpu.VMEM((n_fs * tok, width), BF16),
                pltpu.VMEM((max(depth, LANES), LANES), F32),
                pltpu.VMEM((slots, expert_count, depth, ch), F32),
                pltpu.VMEM((slots, expert_count, depth, ch), F32),
                pltpu.VMEM((n_chunks, expert_count, depth, 2 * ch), BF16),
                pltpu.VMEM((n_chunks, width, 2 * ch), BF16),
                pltpu.VMEM((n_chunks, dcols, n_tp * ch), BF16),
                pltpu.VMEM((n_chunks, n_fs * tok, n_tp * ch), BF16),
                pltpu.VMEM((n_fs * tok, dcols), F32),
                pltpu.VMEM((n_fs, expert_count, tok), F32),
                pltpu.VMEM((n_z, tok, dcols), BF16),
                pltpu.VMEM((n_z, tok, dcols), BF16),
                pltpu.VMEM((n_z, tok, dcols), BF16),
                pltpu.VMEM((n_z, tok, dcols), BF16),
                dma((2,)), dma((2, slots)), dma((n_chunks,)), dma((2, n_chunks)), dma((n_chunks,)),
            ] + [dma(shape) for shape in pairs for _ in range(2)],
            compiler_params=pltpu.CompilerParams(collective_id=0, has_side_effects=True),
        )(tokens, experts.T, routing.T, lines, gate_master, linear_master, down_weight)

    placed = (
        P("fs", None),
        P("fs", None),
        P("fs", None),
        P(),
        P(None, "fs", "tp"),
        P(None, "fs", "tp"),
        P("fs", None, "tp"),
    )
    return jax.shard_map(
        on_device,
        mesh=mesh,
        in_specs=placed,
        out_specs=(P("fs", None, "tp"), P("fs", None, "tp"), P("fs", "tp")),
        check_vma=False,
    )
```

```python
import functools

import jax
import jax.numpy as jnp
from jax import lax
from jax.experimental import pallas as pl
from jax.experimental.pallas import tpu as pltpu
from jax.sharding import PartitionSpec as P

clamp_limit = 7.0
gate_slope = 1.702
CORES = 2
LANES = 128
MESH = pl.DeviceIdType.MESH
F32, BF16 = jnp.float32, jnp.bfloat16


def loop(lo, hi, body):
    if hi - lo <= 8:
        for k in range(lo, hi):
            body(k)
    else:
        lax.fori_loop(lo, hi, lambda k, c: (body(k), c)[1], 0)


def kernel(
    n_fs, n_tp, n_chunks,
    tokens_ref, experts_ref, routing_ref, gain_ref, gate_ref, linear_ref, down_ref,
    gate_out, linear_out, mix_out,
    toks, gains, stage_g, stage_l, wsend, wrecv, dts, acts, acc, shares,
    osend, orecv, zsend, zrecv,
    local_sem, stage_sem, own_sem, out_sem, dl_sem,
    w_s, w_r, s_s, s_r, t1_s, t1_r, t2_s, t2_r, t3_s, t3_r,
    d_s, d_r, a_s, a_r, o_s, o_r, z_s, z_r,
):
    fs, tp = lax.axis_index("fs"), lax.axis_index("tp")
    n_z = n_fs // CORES
    z, core = fs // CORES, lax.rem(fs, CORES)
    partner = z * CORES + (1 - core)
    across = n_z // 2
    tok, width = tokens_ref.shape
    experts, depth, cols = gate_ref.shape
    qcols = width // n_tp
    dcols = width // n_tp
    ch = cols // n_chunks

    def flip(index, mask):
        out, bit = index, 1
        while bit <= mask:
            if mask & bit:
                out = out + bit - 2 * bit * lax.rem(index // bit, 2)
            bit *= 2
        return out

    def zx(m):
        return flip(z, m)

    def ds(i, n):
        return pl.ds(pl.multiple_of(i * n, n), n)

    def remote(src, dst, ss, rs, where):
        return pltpu.make_async_remote_copy(
            src_ref=src, dst_ref=dst, send_sem=ss, recv_sem=rs,
            device_id=where, device_id_type=MESH,
        )

    def peer_fs(k):
        return {"fs": lax.rem(fs + k, n_fs), "tp": tp}

    def peer_tp(k):
        return {"fs": fs, "tp": lax.rem(tp + k, n_tp)}

    over = {"fs": partner, "tp": tp}

    def stage(j):
        slot = j % 2
        c = pl.ds(j * ch, ch)
        return (
            pltpu.make_async_copy(gate_ref.at[:, :, c], stage_g.at[slot], stage_sem.at[0, slot]),
            pltpu.make_async_copy(linear_ref.at[:, :, c], stage_l.at[slot], stage_sem.at[1, slot]),
        )

    def src_fs(m):
        return zx(m) * CORES + core

    def w_copy(j, k):
        to = flip(fs, k)
        return remote(
            wsend.at[j, to], wrecv.at[j, ds(fs, depth)], w_s.at[j, k], w_r.at[j, k], {"fs": to, "tp": tp}
        )

    def w_own(j):
        return pltpu.make_async_copy(wsend.at[j, fs], wrecv.at[j, ds(fs, depth)], own_sem.at[j])

    def s_copy(k):
        return remote(shares.at[fs], shares.at[fs], s_s.at[k], s_r.at[k], peer_fs(k))

    def t1_copy(m):
        block = toks.at[ds(fs if m <= across else src_fs(across), tok), ds(tp, qcols)]
        to = m if m <= across else m - across
        return remote(block, block, t1_s.at[m], t1_r.at[m], {"fs": src_fs(to), "tp": tp})

    def t2_copy(kz, k):
        block = toks.at[ds(src_fs(kz), tok), ds(tp, qcols)]
        return remote(block, block, t2_s.at[kz, k], t2_r.at[kz, k], peer_tp(k))

    def t3_copy(kz):
        block = toks.at[ds(src_fs(kz), tok)]
        return remote(block, block, t3_s.at[kz], t3_r.at[kz], over)

    def d_copy(j, k):
        to = lax.rem(tp + k, n_tp)
        return remote(
            down_ref.at[0, ds(to, dcols), pl.ds(j * ch, ch)],
            dts.at[j, :, ds(tp, ch)], d_s.at[j, k], d_r.at[j, k], peer_tp(k),
        )

    def d_own(j):
        return pltpu.make_async_copy(
            down_ref.at[0, ds(tp, dcols), pl.ds(j * ch, ch)], dts.at[j, :, ds(tp, ch)], dl_sem.at[j]
        )

    def outs(j):
        c = pl.ds(j * ch, ch)
        return (
            pltpu.make_async_copy(wrecv.at[j, :, pl.ds(0, ch)], gate_out.at[0, :, c], out_sem.at[0, j]),
            pltpu.make_async_copy(wrecv.at[j, :, pl.ds(ch, ch)], linear_out.at[0, :, c], out_sem.at[1, j]),
        )

    def o_copy(kz):
        return remote(osend.at[kz], orecv.at[kz], o_s.at[kz], o_r.at[kz], over)

    def a_copy(j, m, k):
        block = acts.at[j, ds(zx(m), CORES * tok), ds(tp, ch)]
        return remote(block, block, a_s.at[j, m, k], a_r.at[j, m, k], peer_tp(k))

    def z_copy(m):
        where = {"fs": zx(m) * CORES + core, "tp": tp}
        return remote(zsend.at[m], zrecv.at[m], z_s.at[m], z_r.at[m], where)

    own_tokens = pltpu.make_async_copy(tokens_ref, toks.at[ds(fs, tok)], local_sem.at[0])
    for c in (own_tokens, *stage(0)):
        c.start()

    barrier = pltpu.get_barrier_semaphore()
    loop(1, n_fs, lambda k: pl.semaphore_signal(barrier, inc=1, device_id=peer_fs(k), device_id_type=MESH))
    loop(1, n_tp, lambda k: pl.semaphore_signal(barrier, inc=1, device_id=peer_tp(k), device_id_type=MESH))

    expert = lax.broadcasted_iota(jnp.int32, (experts, tok), 0)
    share = jnp.zeros((experts, tok), F32)
    for k in range(experts_ref.shape[0]):
        share += jnp.where(experts_ref[k : k + 1, :] == expert, routing_ref[k : k + 1, :], 0.0)
    shares[fs] = share
    for i in range(max(depth // LANES, 1)):
        line = gain_ref[pl.ds(fs * depth // LANES + i, 1), :]
        gains[i * LANES : (i + 1) * LANES, :] = jnp.transpose(jnp.broadcast_to(line, (LANES, LANES)))
    gain_rows = pl.ds(pl.multiple_of(lax.rem(fs * depth, LANES), 8), depth)
    pl.semaphore_wait(barrier, n_fs + n_tp - 2)

    own_tokens.wait()
    for m in range(across, 0, -1):
        t1_copy(m).start()
    early = (n_chunks + 1) // 2
    for j in range(early):
        d_own(j).start()
        loop(1, n_tp, lambda k: d_copy(j, k).start())

    loop(1, n_fs, lambda k: s_copy(k).start())
    half = n_fs // 2

    def prepare(j):
        for c in stage(j):
            c.wait()
        if j + 1 < n_chunks:
            for c in stage(j + 1):
                c.start()

        def cast(e, carry):
            wsend[j, e, :, 0:ch] = (stage_g[j % 2, e] * gains[gain_rows, 0:ch]).astype(BF16)
            wsend[j, e, :, ch:] = (stage_l[j % 2, e] * gains[gain_rows, 0:ch]).astype(BF16)
            return carry

        lax.fori_loop(0, experts, cast, 0)
        w_own(j).start()
        for k in range(half - 1, 0, -1):
            w_copy(j, k).start()

    def spread(m):
        t1_copy(m).wait_recv()
        loop(1, n_tp, lambda k: t2_copy(m, k).start())

    crossing = list(range(n_fs - 1, half - 1, -1))
    prepare(0)
    for k in crossing[: half // 2]:
        w_copy(0, k).start()
    spread(across)
    for m in range(across + 1, n_z):
        t1_copy(m).start()
    for k in crossing[half // 2 :]:
        w_copy(0, k).start()
    t3_copy(0).start()
    for m in range(1, across):
        spread(m)
    for js in ([1], list(range(2, n_chunks))):
        for j in js:
            if j < n_chunks:
                prepare(j)
        for j in js:
            for k in crossing:
                if j < n_chunks:
                    w_copy(j, k).start()
    for m in range(across + 1, n_z):
        spread(m)
    for j in range(early, n_chunks):
        d_own(j).start()
        loop(1, n_tp, lambda k: d_copy(j, k).start())
    for m in range(1, n_z):
        loop(1, n_tp, lambda k: t2_copy(m, k).wait_recv())
        t3_copy(m).start()
    for m in range(n_z):
        t3_copy(m).wait_recv()

    total = n_fs * tok
    rows = min(total, 256)

    def down(j):
        d_own(j).wait()
        loop(1, n_tp, lambda k: d_copy(j, k).wait_recv())

    def product(j, r):
        return lax.dot_general(
            acts[j, r, :], dts[j], (((1,), (1,)), ((), ())), preferred_element_type=F32
        )

    def gathered(j, m):
        loop(1, n_tp, lambda k: a_copy(j, m, k).wait_recv())

    def accumulate(j):
        down(j)
        for m in range(n_z):
            gathered(j, m)

        def step(i, carry):
            r = ds(i, rows)
            if j == 0:
                acc[r, :] = product(j, r)
            else:
                acc[r, :] += product(j, r)
            return carry

        lax.fori_loop(0, total // rows, step, 0)

    def arrive(j):
        w_own(j).wait()
        for k in range(1, n_fs):
            w_copy(j, k).wait_recv()
        for c in outs(j):
            c.start()

    def up(j, r):
        pre = jnp.dot(toks[r, :], wrecv[j], preferred_element_type=F32)
        c = jnp.minimum(pre[:, 0:ch], clamp_limit)
        lin = jnp.clip(pre[:, ch:], -clamp_limit, clamp_limit) + 1.0
        acts[j, r, ds(tp, ch)] = (c * jax.nn.sigmoid(gate_slope * c) * lin).astype(BF16)

    last = n_chunks - 1
    order = list(range(n_z - 1, -1, -1))
    for j in range(n_chunks):
        arrive(j)
        for m in order:
            up(j, ds(zx(m), CORES * tok))
            loop(1, n_tp, lambda k: a_copy(j, m, k).start())
        if j > 0:
            accumulate(j - 1)

    loop(1, n_fs, lambda k: s_copy(k).wait_recv())
    down(last)

    def weighted(who):
        r = ds(who, tok)
        value = product(last, r)
        if last > 0:
            value = value + acc[r, :]
        line = shares[who, pl.ds(fs, 1), :]
        w = jnp.transpose(jnp.broadcast_to(line, (tok, tok)))
        return value * jnp.concatenate([w] * (dcols // LANES), axis=1)

    def pass_on(m):
        r = ds(zx(m) * CORES + core, tok)
        o_copy(m).wait_recv()
        if m == 0:
            acc[r, :] += orecv[m].astype(F32)
        else:
            zsend[m] = (acc[r, :] + orecv[m].astype(F32)).astype(BF16)
            z_copy(m).start()

    for m in order:
        gathered(last, m)
        osend[m] = weighted(zx(m) * CORES + (1 - core)).astype(BF16)
        o_copy(m).start()
        kept = zx(m) * CORES + core
        acc[ds(kept, tok), :] = weighted(kept)
        if m < n_z - 1:
            pass_on(m + 1)
    pass_on(0)
    r = ds(fs, tok)
    for m in order[:-1]:
        z_copy(m).wait_recv()
        acc[r, :] += zrecv[m].astype(F32)
    mix_out[...] = acc[r, :].astype(BF16)

    for j in range(n_chunks):
        for c in outs(j):
            c.wait()
        for k in range(1, n_fs):
            w_copy(j, k).wait_send()
        loop(1, n_tp, lambda k: d_copy(j, k).wait_send())
        for m in order:
            loop(1, n_tp, lambda k: a_copy(j, m, k).wait_send())
    loop(1, n_fs, lambda k: s_copy(k).wait_send())
    for m in range(n_z):
        if m > 0:
            t1_copy(m).wait_send()
            loop(1, n_tp, lambda k: t2_copy(m, k).wait_send())
        t3_copy(m).wait_send()
    loop(0, n_z, lambda kz: o_copy(kz).wait_send())
    for m in order[:-1]:
        z_copy(m).wait_send()


def solution(mesh):
    n_fs, n_tp = mesh.shape["fs"], mesh.shape["tp"]

    def on_device(tokens, experts, routing, norm_gain, gate_master, linear_master, down_weight):
        expert_count, depth, cols = gate_master.shape
        tok, width = tokens.shape
        n_z = n_fs // CORES
        ch = min(LANES, cols)
        n_chunks = cols // ch
        dcols = width // n_tp
        lines = norm_gain.reshape(width // LANES, LANES)
        hbm = pl.BlockSpec(memory_space=pl.ANY)
        vmem = pl.BlockSpec(memory_space=pltpu.VMEM)
        dma = pltpu.SemaphoreType.DMA
        slots = min(2, n_chunks)
        out_shape = jax.ShapeDtypeStruct((1, width, cols), BF16)
        pairs = [
            (n_chunks, n_fs), (n_fs,), (n_z,), (n_z, n_tp), (n_z,),
            (n_chunks, n_tp), (n_chunks, n_z, n_tp), (n_z,), (n_z,),
        ]
        return pl.pallas_call(
            functools.partial(kernel, n_fs, n_tp, n_chunks),
            out_shape=(out_shape, out_shape, jax.ShapeDtypeStruct((tok, dcols), BF16)),
            in_specs=[hbm, vmem, vmem, vmem, hbm, hbm, hbm],
            out_specs=(hbm, hbm, vmem),
            scratch_shapes=[
                pltpu.VMEM((n_fs * tok, width), BF16),
                pltpu.VMEM((max(depth, LANES), LANES), F32),
                pltpu.VMEM((slots, expert_count, depth, ch), F32),
                pltpu.VMEM((slots, expert_count, depth, ch), F32),
                pltpu.VMEM((n_chunks, expert_count, depth, 2 * ch), BF16),
                pltpu.VMEM((n_chunks, width, 2 * ch), BF16),
                pltpu.VMEM((n_chunks, dcols, n_tp * ch), BF16),
                pltpu.VMEM((n_chunks, n_fs * tok, n_tp * ch), BF16),
                pltpu.VMEM((n_fs * tok, dcols), F32),
                pltpu.VMEM((n_fs, expert_count, tok), F32),
                pltpu.VMEM((n_z, tok, dcols), BF16),
                pltpu.VMEM((n_z, tok, dcols), BF16),
                pltpu.VMEM((n_z, tok, dcols), BF16),
                pltpu.VMEM((n_z, tok, dcols), BF16),
                dma((2,)), dma((2, slots)), dma((n_chunks,)), dma((2, n_chunks)), dma((n_chunks,)),
            ] + [dma(shape) for shape in pairs for _ in range(2)],
            compiler_params=pltpu.CompilerParams(collective_id=0, has_side_effects=True),
        )(tokens, experts.T, routing.T, lines, gate_master, linear_master, down_weight)

    placed = (
        P("fs", None),
        P("fs", None),
        P("fs", None),
        P(),
        P(None, "fs", "tp"),
        P(None, "fs", "tp"),
        P("fs", None, "tp"),
    )
    return jax.shard_map(
        on_device,
        mesh=mesh,
        in_specs=placed,
        out_specs=(P("fs", None, "tp"), P("fs", None, "tp"), P("fs", "tp")),
        check_vma=False,
    )
```
